32 devices in a mesh: fs: 8 (over z, y), tp: 4 (over x, core).
Axes of the slice: x: 2, y: 2, z: 4, core: 2. Of those that a mesh axis runs over, the one named last changes fastest.
Arguments:
- late_input: bfloat16 [2048, 2048], P(('fs', 'tp')), may hold values from -6 to 6
- early_input: bfloat16 [2048, 2048], P(('fs', 'tp')), may hold values from -6 to 6
- early_grad: bfloat16 [2048, 2048], P(('fs', 'tp')), may hold values from -6 to 6
- pre_gain: float32 [2048], replicated, may hold values from 0.1 to 1.9
- post_gain: float32 [2048], replicated, may hold values from 0.1 to 1.9
- gate_weight: bfloat16 [2048, 4096], P('fs', 'tp'), may hold values from -0.125 to 0.125
- up_weight: bfloat16 [2048, 4096], P('fs', 'tp'), may hold values from -0.125 to 0.125
- down_weight: bfloat16 [2048, 4096], P('fs', 'tp'), may hold values from -0.09375 to 0.09375
- gate_sum: float32 [2048, 4096], P('fs', 'tp'), may hold values from -1.8 to 1.8
- up_sum: float32 [2048, 4096], P('fs', 'tp'), may hold values from -1.8 to 1.8
- down_gradient_sum: float32 [2048, 4096], P('fs', 'tp'), may hold values from -1.8 to 1.8
Outputs:
- late_output: bfloat16 [2048, 2048], P(('fs', 'tp'))
- early_input_grad: bfloat16 [2048, 2048], P(('fs', 'tp'))
- gate_total: float32 [2048, 4096], P('fs', 'tp')
- up_total: float32 [2048, 4096], P('fs', 'tp')
- down_total: float32 [2048, 4096], P('fs', 'tp')
The draws below stay inside these ranges and needn't reach their ends.
All inputs are finite; a program needn't handle non-finite values.
Results may differ from the reference program's by a relative error of at most 0.013.
Values may be sent and summed in bfloat16 or wider, within the bound.
A program may use at most 128 MiB of HBM per device.

```python
import math
import jax
import jax.numpy as jnp
from jax import lax

D = 2048
FF = 4096
ROWS = 2048
N_TP = 4


def with_spikes(array, rng, source, target, shards_of, factor):
    def block_of(position):
        return (jnp.arange(array.shape[position]) // (array.shape[position] // shards_of)).reshape((-1,) + (1,) * (array.ndim - 1 - position))

    one_side = jax.random.permutation(rng, shards_of)[block_of(target)]
    other_side = (block_of(target) + shards_of // 2) % shards_of
    return jnp.where((block_of(source) == one_side) | (block_of(source) == other_side), factor * array, array)


def shard_levels(own_key, shape, pieces, least, top_value):
    gain, own = 1.0, jax.random.fold_in(own_key, 6)
    for dim, shards_of in pieces:
        draws = jnp.exp(jax.random.uniform(jax.random.fold_in(own, dim), (shards_of,), jnp.float32, least / len(pieces), top_value / len(pieces)))
        gain = gain * jnp.repeat(draws, shape[dim] // shards_of).reshape([-1 if axis == dim else 1 for axis in range(len(shape))])
    return gain


def gaussian(rng, shape, scale, bound, split=(), held_as=jnp.bfloat16):
    loudness = shard_levels(rng, shape, split, -0.22, 0.18) if split else 1.0
    entries = jax.random.normal(rng, shape, jnp.float32) * scale * loudness
    return jnp.minimum(jnp.maximum(entries, -bound), bound).astype(held_as)


def noise_with(stream_key, shape, spread, limit, pieces, heavy, held_as=jnp.bfloat16):
    result = spread * jax.random.normal(stream_key, shape, jnp.float32)
    if pieces:
        result = result * shard_levels(stream_key, shape, pieces, -0.22, 0.18)
    return jnp.clip(with_spikes(result, jax.random.fold_in(stream_key, 3), *heavy), -limit, limit).astype(held_as)


def setup_inputs(seed: int = 0) -> dict:
    seeds = jax.random.split(jax.random.key(seed), 12)
    late_input = gaussian(seeds[0], (ROWS, D), 1.0, 6.0, ((0, 32),))
    early_input = gaussian(seeds[1], (ROWS, D), 1.0, 6.0, ((0, 32),))
    early_grad = noise_with(seeds[2], (ROWS, D), 1.0, 6.0, ((0, 32),), (0, 1, 32, 2.75))
    pre_gain = jnp.clip(1.0 + 0.18 * jax.random.normal(seeds[3], (D,), jnp.float32), 0.1, 1.9)
    post_gain = jnp.clip(1.0 + 0.18 * jax.random.normal(seeds[4], (D,), jnp.float32), 0.1, 1.9)
    gate_weight = gaussian(seeds[5], (D, FF), D ** -0.5, 0.125, ((0, 8), (1, 4)))
    up_weight = gaussian(seeds[6], (D, FF), D ** -0.5, 0.125, ((0, 8), (1, 4)))
    down_weight = gaussian(seeds[7], (D, FF), FF ** -0.5, 0.09375, ((0, 8), (1, 4)))
    gate_sum = gaussian(seeds[8], (D, FF), 0.3, 1.8, ((0, 8), (1, 4)), jnp.float32)
    up_sum = gaussian(seeds[9], (D, FF), 0.3, 1.8, ((0, 8), (1, 4)), jnp.float32)
    down_gradient_sum = gaussian(seeds[10], (D, FF), 0.3, 1.8, ((0, 8), (1, 4)), jnp.float32)
    return dict(late_input=late_input, early_input=early_input, early_grad=early_grad, pre_gain=pre_gain, post_gain=post_gain, gate_weight=gate_weight, up_weight=up_weight, down_weight=down_weight, gate_sum=gate_sum, up_sum=up_sum, down_gradient_sum=down_gradient_sum)


NORM_EPS = 1e-06

def contract_last(first_op, second_op):
    return lax.dot_general(first_op, second_op, (((1,), (1,)), ((), ())), preferred_element_type=jnp.float32)

def contract_first(first_op, second_op):
    return lax.dot_general(first_op, second_op, (((0,), (0,)), ((), ())), preferred_element_type=jnp.float32)

def inverse_rms(values):
    return lax.rsqrt(lax.optimization_barrier(jnp.mean(values * values, axis=-1, keepdims=True)) + NORM_EPS)

def rounded_blocks(term_of, row_count):
    running = jnp.zeros((row_count, D), jnp.float32)
    for block_index in range(N_TP):
        rounded = lax.optimization_barrier(term_of(block_index).astype(jnp.bfloat16))
        running = running + rounded.astype(jnp.float32)
    return running.astype(jnp.bfloat16)

def forward_rows(input_rows, pre_gain, gate_weight, up_weight, down_weight):
    values = input_rows.astype(jnp.float32)
    normed = (values * inverse_rms(values) * pre_gain).astype(jnp.bfloat16)
    gate_pre = jnp.dot(normed, gate_weight, preferred_element_type=jnp.float32)
    up_pre = jnp.dot(normed, up_weight, preferred_element_type=jnp.float32)
    hidden_state = (jax.nn.silu(gate_pre) * up_pre).astype(jnp.bfloat16)
    block_column_count = FF // N_TP

    def term_of(block_index):
        columns = slice(block_index * block_column_count, (block_index + 1) * block_column_count)
        return contract_last(hidden_state[:, columns], down_weight[:, columns])
    mixed = rounded_blocks(term_of, input_rows.shape[0])
    return (normed, gate_pre, up_pre, hidden_state, mixed)

def reference(late_input, early_input, early_grad, pre_gain, post_gain, gate_weight, up_weight, down_weight, gate_sum, up_sum, down_gradient_sum):
    late_mixed = forward_rows(late_input, pre_gain, gate_weight, up_weight, down_weight)[4]
    late_values = late_input.astype(jnp.float32)
    mixed_values = late_mixed.astype(jnp.float32)
    late_output = (late_values + 0.5 * mixed_values * inverse_rms(mixed_values) * post_gain).astype(jnp.bfloat16)
    normed, gate_pre, up_pre, hidden_state, mixed = forward_rows(early_input, pre_gain, gate_weight, up_weight, down_weight)
    early_mixed = mixed.astype(jnp.float32)
    inverse_norm = inverse_rms(early_mixed)
    weighted = 0.5 * early_grad.astype(jnp.float32) * post_gain
    mixed_cot = (inverse_norm * weighted - early_mixed * inverse_norm ** 3 * lax.optimization_barrier(jnp.mean(weighted * early_mixed, axis=-1, keepdims=True))).astype(jnp.bfloat16)
    hidden_cot = jnp.dot(mixed_cot, down_weight, preferred_element_type=jnp.float32)
    sigmoid_gate = jax.nn.sigmoid(gate_pre)
    gate_cot = (hidden_cot * up_pre * sigmoid_gate * (1.0 + gate_pre * (1.0 - sigmoid_gate))).astype(jnp.bfloat16)
    up_cot = (hidden_cot * gate_pre * sigmoid_gate).astype(jnp.bfloat16)
    block_column_count = FF // N_TP

    def back_term(block_index):
        columns = slice(block_index * block_column_count, (block_index + 1) * block_column_count)
        return contract_last(gate_cot[:, columns], gate_weight[:, columns]) + contract_last(up_cot[:, columns], up_weight[:, columns])
    normed_cot = rounded_blocks(back_term, early_input.shape[0]).astype(jnp.float32)
    early_values = early_input.astype(jnp.float32)
    early_inverse_norm = inverse_rms(early_values)
    weighted_in = normed_cot * pre_gain
    early_input_grad = (early_grad.astype(jnp.float32) + early_inverse_norm * weighted_in - early_values * early_inverse_norm ** 3 * lax.optimization_barrier(jnp.mean(weighted_in * early_values, axis=-1, keepdims=True))).astype(jnp.bfloat16)
    grad_scale = 1.0 / math.sqrt(ROWS)
    gate_total = gate_sum + grad_scale * contract_first(normed, gate_cot)
    up_total = up_sum + grad_scale * contract_first(normed, up_cot)
    down_total = down_gradient_sum + grad_scale * contract_first(mixed_cot, hidden_state)
    return (late_output, early_input_grad, gate_total, up_total, down_total)
```

```python
import functools
import math

import jax
import jax.numpy as jnp
from jax import lax
from jax.experimental import pallas as pl
from jax.experimental.pallas import tpu as pltpu
from jax.sharding import PartitionSpec as P

NORM_EPS = 1e-06
PAIR = 2
GROUP = 16
LATE, EARLY = 0, 1
GATE, UP, DOWN = 0, 1, 2
MESH = pl.DeviceIdType.MESH
VMEM_LIMIT = 60 * 1024 * 1024
BF16, F32 = jnp.bfloat16, jnp.float32


def contract_last(first_op, second_op):
    return lax.dot_general(
        first_op, second_op, (((1,), (1,)), ((), ())), preferred_element_type=F32
    )


def contract_first(first_op, second_op):
    return lax.dot_general(
        first_op, second_op, (((0,), (0,)), ((), ())), preferred_element_type=F32
    )


def inverse_rms(values):
    return lax.rsqrt(jnp.mean(values * values, axis=-1, keepdims=True) + NORM_EPS)


def quad_of(n_fs, n_tp):
    return min(n_fs, max(1, GROUP // n_tp))


class Place:
    def __init__(self, n_fs, n_tp):
        self.n_fs, self.n_tp = n_fs, n_tp
        self.quad = quad_of(n_fs, n_tp)
        self.groups, self.xs = n_fs // self.quad, n_tp // PAIR
        self.fs, self.tp = lax.axis_index("fs"), lax.axis_index("tp")
        self.g, self.q = self.fs // self.quad, self.fs % self.quad
        self.x, self.core = self.tp // PAIR, self.tp % PAIR
        self.me = self.member(0, 0, self.core)
        self.partner = self.device(0, 0, 1 - self.core)

    def at_q(self, dq):
        return (self.q + self.quad + dq) % self.quad

    def at_x(self, dx):
        return (self.x + self.xs + dx) % self.xs

    def at_g(self, dg):
        return (self.g + dg) % self.groups

    def member(self, dq, dx, core):
        return self.at_q(dq) * self.n_tp + self.at_x(dx) * PAIR + core

    def device(self, dq, dx, core):
        return {"fs": self.g * self.quad + self.at_q(dq), "tp": self.at_x(dx) * PAIR + core}

    def slot(self, dg, dq):
        return self.at_g(dg) * self.quad + self.at_q(dq)

    def enter(self):
        barrier = pltpu.get_barrier_semaphore()

        def greet(fs, tp):
            pl.semaphore_signal(
                barrier, inc=1, device_id={"fs": fs, "tp": tp}, device_id_type=MESH
            )

        peers = 0
        for offset in range(1, self.n_fs):
            greet((self.fs + offset) % self.n_fs, self.tp)
            peers += 1
        for dq in range(self.quad):
            for offset in range(1, self.n_tp):
                greet(self.g * self.quad + self.at_q(dq), (self.tp + offset) % self.n_tp)
                peers += 1
        pl.semaphore_wait(barrier, peers)


def remote(src, dst, send_sem, recv_sem, who):
    return pltpu.make_async_remote_copy(
        src_ref=src,
        dst_ref=dst,
        send_sem=send_sem,
        recv_sem=recv_sem,
        device_id=who,
        device_id_type=MESH,
    )


def layer_kernel(n_fs, n_tp, grad_scale, *refs):
    late_ref, early_ref, grad_ref, pre_ref, post_ref = refs[:5]
    w_refs = refs[5:8]
    late_out, early_out = refs[8:10]
    grad_outs = refs[10:13]
    normed, weights, gate, up, hidden, cots, parts, pair_in, sums_in, total = refs[13:23]
    gate_cot, up_cot, grad_parts, grad_in = refs[23:27]
    w_send, w_recv, g_send, g_recv, sems = refs[27:]

    at = Place(n_fs, n_tp)
    quad, xs, groups = at.quad, at.xs, at.groups
    tok_rows, width = early_ref.shape
    rows, units = weights.shape[2:]
    tile = n_tp * tok_rows
    everything = pl.ds(0, width)
    chunk = quad * rows
    offsets = [(dq, dx) for dq in range(quad) for dx in range(xs)]
    others = offsets[1:]
    pending = []

    def start(copy):
        copy.start()
        pending.append(copy)

    def w_copy(w, dg, dq):
        source = w_refs[w].at[:, pl.ds(pl.multiple_of(at.at_q(dq) * units, units), units)]
        who = {"fs": at.slot(dg, dq), "tp": at.tp}
        return remote(
            source, weights.at[w, at.fs], w_send.at[w, dg, dq], w_recv.at[w, dg, dq], who
        )

    q_order = [2, 1, 3, 0] if quad == 4 else list(range(quad - 1, -1, -1))

    def send_weights(w):
        for dq in q_order:
            for dg in range(groups - 1, -1, -1):
                if dg or dq:
                    start(w_copy(w, dg, dq))

    def wait_weights(w, dgs):
        for dg in dgs:
            for dq in q_order:
                if dg or dq:
                    w_copy(w, dg, dq).wait_recv()

    def all_rows(w):
        return weights[w].reshape(n_fs * rows, units)

    def ici(inst, dq, dx, src, dst, who):
        return remote(src, dst, sems.at[inst, 0, dq, dx], sems.at[inst, 1, dq, dx], who)

    def pair(inst, dq, dx, src, dst):
        return remote(src, dst, sems.at[inst, 2, dq, dx], sems.at[inst, 3, dq, dx], at.partner)

    def gather_copy(inst, buf, dq, dx, direct):
        if direct or dx == 0:
            block = buf.at[at.me]
            return ici(inst, dq, dx, block, block, at.device(dq, dx, at.core))
        block = buf.at[at.member(-dq, 0, at.core)]
        return ici(inst, dq, dx, block, block, at.device(0, dx, at.core))

    def gather_pair(inst, buf, dq, dx):
        block = buf.at[at.member(-dq, -dx, at.core)]
        return pair(inst, dq, dx, block, block)

    def gather_start(inst, buf, direct):
        for dq, dx in others:
            if direct or dq == 0 or dx == 0:
                start(gather_copy(inst, buf, dq, dx, direct))
        start(gather_pair(inst, buf, 0, 0))

    def gather_pass_on(inst, buf, direct):
        if not direct:
            for dq in range(1, quad):
                gather_copy(inst, buf, dq, 0, direct).wait_recv()
                for dx in range(1, xs):
                    start(gather_copy(inst, buf, dq, dx, direct))
                start(gather_pair(inst, buf, dq, 0))
        for dq, dx in others:
            if direct or dx:
                gather_copy(inst, buf, dq, dx, direct).wait_recv()
                start(gather_pair(inst, buf, dq, dx))

    def gather_wait(inst, buf):
        for dq, dx in offsets:
            gather_pair(inst, buf, dq, dx).wait_recv()

    def sum_pair(inst, held, cols, dq, dx):
        return pair(
            inst,
            dq,
            dx,
            parts.at[held, at.member(dq, dx, 1 - at.core), :, cols],
            pair_in.at[held, dq, dx, :, cols],
        )

    def sum_copy(inst, held, cols, dq, dx, direct):
        if direct:
            who = at.device(dq, dx, at.core)
        else:
            who = at.device(0, dx, at.core) if dx else at.device(dq, 0, at.core)
        return ici(
            inst,
            dq,
            dx,
            parts.at[held, at.member(dq, dx, at.core), :, cols],
            sums_in.at[held, dq, dx, :, cols],
            who,
        )

    def sum_start(inst, held, cols, direct, compute):
        def reduce_pairs(dq):
            for dx in list(range(1, xs)) + [0]:
                sum_pair(inst, held, cols, dq, dx).wait_recv()
                mine = at.member(dq, dx, at.core)
                both = parts[held, mine, :, cols].astype(F32) + pair_in[
                    held, dq, dx, :, cols
                ].astype(F32)
                if direct and dq == 0 and dx == 0:
                    total[:, cols] = both
                    continue
                parts[held, mine, :, cols] = both.astype(BF16)
                if direct or dx:
                    start(sum_copy(inst, held, cols, dq, dx, direct))

        ready = None
        for dq in list(range(1, quad)) + [0]:
            compute(at.at_q(dq))
            for dx in range(xs):
                start(sum_pair(inst, held, cols, dq, dx))
            if ready is not None:
                reduce_pairs(ready)
            ready = dq
        reduce_pairs(ready)

    def sum_pass_on(inst, held, cols):
        for dq in list(range(1, quad)) + [0]:
            mine = at.member(dq, 0, at.core)
            running = parts[held, mine, :, cols].astype(F32)
            for dx in range(1, xs):
                sum_copy(inst, held, cols, dq, dx, False).wait_recv()
                running = running + sums_in[held, dq, dx, :, cols].astype(F32)
            if dq:
                parts[held, mine, :, cols] = running.astype(BF16)
                start(sum_copy(inst, held, cols, dq, 0, False))
            else:
                total[:, cols] = running

    def sum_finish(inst, held, cols, direct):
        for dq, dx in others:
            if direct or dx == 0:
                sum_copy(inst, held, cols, dq, dx, direct).wait_recv()
                total[:, cols] += sums_in[held, dq, dx, :, cols].astype(F32)

    def by_owner(product):
        return product.astype(BF16).reshape(n_tp, tok_rows, product.shape[-1])

    def span_of(q):
        return pl.ds(pl.multiple_of(q * tile, tile), tile)

    def members_of(q):
        return pl.ds(q * n_tp, n_tp)

    def normalise(part, src):
        values = src[...].astype(F32)
        normed[part, at.me] = (values * inverse_rms(values) * pre_ref[...]).astype(BF16)

    def activations(part, q):
        tokens = normed[part, members_of(q)].reshape(tile, width)
        gate_tile = jnp.dot(tokens, all_rows(GATE), preferred_element_type=F32)
        up_tile = jnp.dot(tokens, all_rows(UP), preferred_element_type=F32)
        return gate_tile, up_tile, (gate_tile * jax.nn.sigmoid(gate_tile) * up_tile).astype(BF16)

    early_tokens, late_tokens, cot_tokens, normed_sum, late_sum, mixed_sum = range(6)

    at.enter()
    normalise(EARLY, early_ref)
    gather_start(early_tokens, normed.at[EARLY], False)
    send_weights(GATE)
    normalise(LATE, late_ref)
    gather_start(late_tokens, normed.at[LATE], False)
    send_weights(UP)
    send_weights(DOWN)
    for w in range(3):
        own = pl.ds(pl.multiple_of(at.q * units, units), units)
        weights[w, at.fs] = w_refs[w][:, own]
    gather_pass_on(early_tokens, normed.at[EARLY], False)
    gather_pass_on(late_tokens, normed.at[LATE], False)
    gather_wait(early_tokens, normed.at[EARLY])
    wait_weights(GATE, range(groups))
    wait_weights(UP, range(groups))

    @pl.loop(0, quad)
    def _(i):
        span = span_of(i)
        gate[span], up[span], hidden[span] = activations(EARLY, i)

    def chunk_of(dg):
        return pl.ds(pl.multiple_of(at.at_g(dg) * chunk, chunk), chunk)

    first_mixed = len(pending)
    for dg in range(groups):
        wait_weights(DOWN, [dg])

        def mixed_part(q, dg=dg):
            down = weights[DOWN, pl.ds(at.at_g(dg) * quad, quad)].reshape(chunk, units)
            parts[0, members_of(q), :, chunk_of(dg)] = by_owner(
                contract_last(hidden[span_of(q)], down)
            )

        sum_start(mixed_sum + dg, 0, chunk_of(dg), True, mixed_part)
    mixed_sends = pending[first_mixed:]
    del pending[first_mixed:]
    for dg in range(groups):
        sum_finish(mixed_sum + dg, 0, chunk_of(dg), True)
    mixed = total[...].astype(BF16).astype(F32)
    inverse = inverse_rms(mixed)
    weighted = 0.5 * grad_ref[...].astype(F32) * post_ref[...]
    cots[at.me] = (
        inverse * weighted
        - mixed * inverse**3 * jnp.mean(weighted * mixed, axis=-1, keepdims=True)
    ).astype(BF16)
    gather_start(cot_tokens, cots, True)
    gather_pass_on(cot_tokens, cots, True)
    gather_wait(cot_tokens, cots)

    def grad_copy(w, dg, dq):
        slot = at.slot(dg, dq)
        who = {"fs": slot, "tp": at.tp}
        return remote(
            grad_parts.at[w, slot],
            grad_in.at[w, dg, dq],
            g_send.at[w, dg, dq],
            g_recv.at[w, dg, dq],
            who,
        )

    def grad_part(w, left_ref, right_ref, dg):
        @pl.loop(0, quad)
        def _(dq):
            slot = at.slot(dg, dq)
            left = left_ref[:, :, pl.ds(pl.multiple_of(slot * rows, rows), rows)]
            left = left.reshape(quad * tile, rows)
            grad_parts[w, slot] = (grad_scale * contract_first(left, right_ref[...])).astype(BF16)

        for dq in q_order:
            if dg or dq:
                start(grad_copy(w, dg, dq))

    early_rows = normed.at[EARLY]
    for dg in range(1, groups):
        grad_part(DOWN, cots, hidden, dg)

    @pl.loop(0, quad)
    def _(i):
        span = span_of(i)
        cot = cots[members_of(i)].reshape(tile, width)
        hidden_cot = jnp.dot(cot, all_rows(DOWN), preferred_element_type=F32)
        gate_tile, up_tile = gate[span], up[span]
        sigmoid = jax.nn.sigmoid(gate_tile)
        gate_cot[span] = (
            hidden_cot * up_tile * sigmoid * (1.0 + gate_tile * (1.0 - sigmoid))
        ).astype(BF16)
        up_cot[span] = (hidden_cot * gate_tile * sigmoid).astype(BF16)

    for dg in range(1, groups):
        grad_part(GATE, early_rows, gate_cot, dg)
        grad_part(UP, early_rows, up_cot, dg)
    grad_part(DOWN, cots, hidden, 0)
    grad_part(GATE, early_rows, gate_cot, 0)
    grad_part(UP, early_rows, up_cot, 0)

    def normed_part(q):
        span = span_of(q)
        parts[1, members_of(q)] = by_owner(
            contract_last(gate_cot[span], all_rows(GATE))
            + contract_last(up_cot[span], all_rows(UP))
        )

    sum_start(normed_sum, 1, everything, False, normed_part)

    for copy in mixed_sends:
        copy.wait_send()
    gather_wait(late_tokens, normed.at[LATE])

    def late_part(q):
        parts[0, members_of(q)] = by_owner(
            contract_last(activations(LATE, q)[2], all_rows(DOWN))
        )

    sum_start(late_sum, 0, everything, False, late_part)
    sum_pass_on(normed_sum, 1, everything)
    sum_finish(normed_sum, 1, everything, False)
    values = early_ref[...].astype(F32)
    inverse = inverse_rms(values)
    weighted = total[...].astype(BF16).astype(F32) * pre_ref[...]
    early_out[...] = (
        grad_ref[...].astype(F32)
        + inverse * weighted
        - values * inverse**3 * jnp.mean(weighted * values, axis=-1, keepdims=True)
    ).astype(BF16)
    sum_pass_on(late_sum, 0, everything)
    sum_finish(late_sum, 0, everything, False)
    mixed = total[...].astype(BF16).astype(F32)
    late_out[...] = (
        late_ref[...].astype(F32) + 0.5 * mixed * inverse_rms(mixed) * post_ref[...]
    ).astype(BF16)

    for w in (DOWN, GATE, UP):
        for dq in q_order:
            running = None
            for dg in range(groups):
                if dg or dq:
                    grad_copy(w, dg, dq).wait_recv()
                    term = grad_in[w, dg, dq].astype(F32)
                else:
                    term = grad_parts[w, at.fs].astype(F32)
                running = term if running is None else running + term
            own = pl.ds(pl.multiple_of(at.at_q(-dq) * units, units), units)
            grad_outs[w][:, own] = running.astype(BF16)

    for copy in pending:
        copy.wait_send()


def per_device(
    n_fs,
    n_tp,
    late_input,
    early_input,
    early_grad,
    pre_gain,
    post_gain,
    gate_weight,
    up_weight,
    down_weight,
    gate_sum,
    up_sum,
    down_gradient_sum,
):
    tok_rows, width = late_input.shape
    rows, hidden_width = gate_weight.shape
    quad = quad_of(n_fs, n_tp)
    groups, xs, members = n_fs // quad, n_tp // PAIR, quad * n_tp
    units = hidden_width // quad
    group_rows = members * tok_rows
    grad_scale = 1.0 / math.sqrt(tok_rows * n_tp * n_fs)
    dma = pltpu.SemaphoreType.DMA
    operands = (
        late_input,
        early_input,
        early_grad,
        pre_gain.reshape(1, width),
        post_gain.reshape(1, width),
        gate_weight,
        up_weight,
        down_weight,
    )
    outs = [jax.ShapeDtypeStruct((tok_rows, width), BF16)] * 2 + [
        jax.ShapeDtypeStruct((rows, hidden_width), BF16)
    ] * 3
    in_vmem = pl.BlockSpec(memory_space=pltpu.VMEM)
    late_output, early_input_grad, *grads = pl.pallas_call(
        functools.partial(layer_kernel, n_fs, n_tp, grad_scale),
        out_shape=outs,
        in_specs=[in_vmem] * len(operands),
        out_specs=[in_vmem] * len(outs),
        scratch_shapes=[
            pltpu.VMEM((2, members, tok_rows, width), BF16),
            pltpu.VMEM((3, n_fs, rows, units), BF16),
            pltpu.VMEM((group_rows, units), F32),
            pltpu.VMEM((group_rows, units), F32),
            pltpu.VMEM((group_rows, units), BF16),
            pltpu.VMEM((members, tok_rows, width), BF16),
            pltpu.VMEM((2, members, tok_rows, width), BF16),
            pltpu.VMEM((2, quad, xs, tok_rows, width), BF16),
            pltpu.VMEM((2, quad, xs, tok_rows, width), BF16),
            pltpu.VMEM((tok_rows, width), F32),
            pltpu.VMEM((group_rows, units), BF16),
            pltpu.VMEM((group_rows, units), BF16),
            pltpu.VMEM((3, n_fs, rows, units), BF16),
            pltpu.VMEM((3, groups, quad, rows, units), BF16),
        ]
        + [dma((3, groups, quad))] * 4
        + [dma((5 + groups, 4, quad, xs))],
        cost_estimate=pl.CostEstimate(flops=10**9, bytes_accessed=0, transcendentals=0),
        compiler_params=pltpu.CompilerParams(
            collective_id=0, has_side_effects=True, vmem_limit_bytes=VMEM_LIMIT
        ),
    )(*operands)
    totals = [
        running + grad.astype(F32)
        for running, grad in zip((gate_sum, up_sum, down_gradient_sum), grads)
    ]
    return (late_output, early_input_grad, *totals)


def solution(mesh):
    in_specs = (
        P(("fs", "tp"), None),
        P(("fs", "tp"), None),
        P(("fs", "tp"), None),
        P(),
        P(),
        P("fs", "tp"),
        P("fs", "tp"),
        P("fs", "tp"),
        P("fs", "tp"),
        P("fs", "tp"),
        P("fs", "tp"),
    )
    out_specs = (
        P(("fs", "tp"), None),
        P(("fs", "tp"), None),
        P("fs", "tp"),
        P("fs", "tp"),
        P("fs", "tp"),
    )
    return jax.shard_map(
        functools.partial(per_device, mesh.shape["fs"], mesh.shape["tp"]),
        mesh=mesh, in_specs=in_specs, out_specs=out_specs, check_vma=False
    )
```

```python
import functools
import math

import jax
import jax.numpy as jnp
from jax import lax
from jax.experimental import pallas as pl
from jax.experimental.pallas import tpu as pltpu
from jax.sharding import PartitionSpec as P

NORM_EPS = 1e-06
PAIR = 2
GROUP = 16
LATE, EARLY = 0, 1
GATE, UP, DOWN = 0, 1, 2
MESH = pl.DeviceIdType.MESH
VMEM_LIMIT = 48 * 1024 * 1024
LANES = 128
BF16, F32 = jnp.bfloat16, jnp.float32
scope = jax.named_scope
LAST_PHASE = (
    "late_send", "down_far", "down_far_crossing", "down_near", "down_near_crossing",
    "down_far_straight", "hidden_cots", "gate_far", "gate_far_crossing", "gate_near",
    "gate_near_crossing", "up_far", "gate_far_straight", "up_far_straight", "normed_start",
    "up_near", "down_near_straight", "gate_near_straight", "late_1", "up_near_crossing",
    "late_2", "normed_1", "up_far_crossing", "up_near_straight", "normed_2", "late_end",
    "normed_end",
)


def contract_last(first_op, second_op):
    return lax.dot_general(
        first_op, second_op, (((1,), (1,)), ((), ())), preferred_element_type=F32
    )


def contract_first(first_op, second_op):
    return lax.dot_general(
        first_op, second_op, (((0,), (0,)), ((), ())), preferred_element_type=F32
    )


def inverse_rms(values):
    return lax.rsqrt(jnp.mean(values * values, axis=-1, keepdims=True) + NORM_EPS)


def quad_of(n_fs, n_tp):
    return min(n_fs, max(1, GROUP // n_tp))


def shape_of(n_fs, n_tp):
    quad = quad_of(n_fs, n_tp)
    deep = PAIR if quad % PAIR == 0 else 1
    return quad // deep, deep, n_tp // PAIR


class Place:
    def __init__(self, n_fs, n_tp):
        self.n_fs, self.n_tp = n_fs, n_tp
        self.quad = quad_of(n_fs, n_tp)
        self.groups = n_fs // self.quad
        self.sizes = shape_of(n_fs, n_tp)
        self.fs, self.tp = lax.axis_index("fs"), lax.axis_index("tp")
        self.g, self.q = self.fs // self.quad, self.fs % self.quad
        self.core = self.tp % PAIR
        self.coords = (self.q // self.sizes[1], self.q % self.sizes[1], self.tp // PAIR)
        self.offsets = [
            (i, j, k)
            for i in range(self.sizes[0])
            for j in range(self.sizes[1])
            for k in range(self.sizes[2])
        ]
        self.me = self.member((0, 0, 0), 1, self.core)
        self.partner = self.device((0, 0, 0), 1 - self.core)

    def moved(self, offset, sign):
        return [
            (c + size + sign * o) % size
            for c, size, o in zip(self.coords, self.sizes, offset)
        ]

    def member(self, offset, sign, core):
        i, j, k = self.moved(offset, sign)
        return (i * self.sizes[1] + j) * self.n_tp + k * PAIR + core

    def device(self, offset, core):
        i, j, k = self.moved(offset, 1)
        return {"fs": self.g * self.quad + i * self.sizes[1] + j, "tp": k * PAIR + core}

    def flat(self, offset):
        return (offset[0] * self.sizes[1] + offset[1]) * self.sizes[2] + offset[2]

    def at_q(self, dq):
        return (self.q + self.quad + dq) % self.quad

    def at_g(self, dg):
        return (self.g + dg) % self.groups

    def slot(self, dg, dq):
        return self.at_g(dg) * self.quad + self.at_q(dq)

    def enter(self):
        barrier = pltpu.get_barrier_semaphore()

        def greet(fs, tp):
            pl.semaphore_signal(
                barrier, inc=1, device_id={"fs": fs, "tp": tp}, device_id_type=MESH
            )

        peers = 0
        for offset in range(1, self.n_fs):
            greet((self.fs + offset) % self.n_fs, self.tp)
            peers += 1
        for dq in range(self.quad):
            for offset in range(1, self.n_tp):
                greet(self.g * self.quad + self.at_q(dq), (self.tp + offset) % self.n_tp)
                peers += 1
        pl.semaphore_wait(barrier, peers)


def remote(src, dst, send_sem, recv_sem, who):
    return pltpu.make_async_remote_copy(
        src_ref=src,
        dst_ref=dst,
        send_sem=send_sem,
        recv_sem=recv_sem,
        device_id=who,
        device_id_type=MESH,
    )


def layer_kernel(n_fs, n_tp, grad_scale, *refs):
    sources = refs[:8]
    late_out, early_out = refs[8:10]
    grad_outs = refs[10:13]
    normed, weights, gate, up, hidden, cots, parts, pair_in, sums_in, total = refs[13:23]
    gate_cot, up_cot, grad_parts, grad_in, hidden_late = refs[23:28]
    late_ref, early_ref, grad_ref, pre_ref, post_ref = refs[28:33]
    w_refs = refs[33:36]
    w_send, w_recv, g_send, g_recv, sems, load_sem = refs[36:]
    loads = [
        pltpu.make_async_copy(src, dst, load_sem.at[i])
        for i, (src, dst) in enumerate(zip(sources, refs[28:36]))
    ]
    for i in (1, 3, 5, 0, 6, 7, 2, 4):
        loads[i].start()

    at = Place(n_fs, n_tp)
    quad, groups, sizes, offsets = at.quad, at.groups, at.sizes, at.offsets
    home, others = offsets[0], offsets[1:]
    tok_rows, width = early_ref.shape
    rows, units = weights.shape[2:]
    tile = n_tp * tok_rows
    chunk = quad * rows
    pending = []

    def start(copy):
        copy.start()
        pending.append(copy)

    def w_copy(w, dg, dq):
        source = w_refs[w].at[:, pl.ds(pl.multiple_of(at.at_q(dq) * units, units), units)]
        who = {"fs": at.slot(dg, dq), "tp": at.tp}
        return remote(
            source, weights.at[w, at.fs], w_send.at[w, dg, dq], w_recv.at[w, dg, dq], who
        )

    q_order = [1, 3, 2, 0] if quad == 4 else list(range(quad - 1, -1, -1))

    def send_weights(w):
        for dq in q_order:
            for dg in range(groups - 1, -1, -1):
                if dg or dq:
                    start(w_copy(w, dg, dq))

    def wait_weights(w, dgs):
        for dg in dgs:
            for dq in q_order:
                if dg or dq:
                    w_copy(w, dg, dq).wait_recv()

    def all_rows(w):
        return weights[w].reshape(n_fs * rows, units)

    def place_in(order, offset, last):
        found = [p for p, axis in enumerate(order) if offset[axis]]
        if not found:
            return -1 if last else len(order)
        return found[-1] if last else found[0]

    def put(offset, axis, value):
        return tuple(value if i == axis else o for i, o in enumerate(offset))

    def along(offset, axis):
        return tuple(o if i == axis else 0 for i, o in enumerate(offset))

    def steps(axis):
        return range(1, sizes[axis])

    def hops(offset):
        return sum(1 for o in offset if o)

    def cols_of(route):
        return pl.ds(route[2], route[3])

    def ici(inst, offset, src, dst, who):
        i = at.flat(offset)
        return remote(src, dst, sems.at[inst, 0, i], sems.at[inst, 1, i], who)

    def pair(inst, offset, src, dst):
        i = at.flat(offset)
        return remote(src, dst, sems.at[inst, 2, i], sems.at[inst, 3, i], at.partner)

    def gather_copy(buf, route, offset):
        axis = route[1][place_in(route[1], offset, True)]
        block = buf.at[at.member(put(offset, axis, 0), -1, at.core), :, cols_of(route)]
        return ici(route[0], offset, block, block, at.device(along(offset, axis), at.core))

    def gather_pair(buf, route, offset):
        block = buf.at[at.member(offset, -1, at.core), :, cols_of(route)]
        return pair(route[0], offset, block, block)

    def onward(route, offset):
        order = route[1]
        later = order[place_in(order, offset, True) + 1 :]
        return [put(offset, axis, e) for axis in later for e in steps(axis)]

    def gather_start(buf, routes):
        sends = [(route, offset) for route in routes for offset in onward(route, home)]
        sends.sort(key=lambda send: place_in(send[0][1], send[1], True))
        for route, offset in sends:
            start(gather_copy(buf, route, offset))
        for route in routes:
            start(gather_pair(buf, route, home))

    def gather_pass_on(buf, routes, stages=range(3)):
        arrivals = [(route, offset) for route in routes for offset in others]
        arrivals = [a for a in arrivals if place_in(a[0][1], a[1], True) in stages]
        arrivals.sort(key=lambda a: (hops(a[1]), place_in(a[0][1], a[1], True)))
        for route, offset in arrivals:
            gather_copy(buf, route, offset).wait_recv()
            for further in onward(route, offset):
                start(gather_copy(buf, route, further))
            start(gather_pair(buf, route, offset))

    def gather_wait(buf, routes):
        for route in routes:
            for offset in offsets:
                gather_pair(buf, route, offset).wait_recv()

    def sum_pair(held, routes, offset):
        cols = pl.ds(routes[0][2], sum(route[3] for route in routes))
        return pair(
            routes[0][0],
            offset,
            parts.at[held, at.member(offset, 1, 1 - at.core), :, cols],
            pair_in.at[held, at.flat(offset), :, cols],
        )

    def sum_copy(held, route, offset):
        axis = route[1][place_in(route[1], offset, False)]
        return ici(
            route[0],
            offset,
            parts.at[held, at.member(offset, 1, at.core), :, cols_of(route)],
            sums_in.at[held, at.flat(offset), :, cols_of(route)],
            at.device(along(offset, axis), at.core),
        )

    def sum_block(held, route, offset):
        cols, mine = cols_of(route), at.member(offset, 1, at.core)
        running = parts[held, mine, :, cols].astype(F32)
        running = running + pair_in[held, at.flat(offset), :, cols].astype(F32)
        for axis in route[1][: place_in(route[1], offset, False)]:
            for e in steps(axis):
                came = put(offset, axis, e)
                sum_copy(held, route, came).wait_recv()
                running = running + sums_in[held, at.flat(came), :, cols].astype(F32)
        if offset == home:
            total[:, cols] = running
        else:
            parts[held, mine, :, cols] = running.astype(BF16)
            start(sum_copy(held, route, offset))

    def sum_send(held, routes, ready):
        for offset in ready:
            sum_pair(held, routes, offset).wait_recv()
        for route in routes:
            for offset in ready:
                if place_in(route[1], offset, False) == 0:
                    sum_block(held, route, offset)

    def sum_start(held, routes, compute, send=True):
        ready = []
        for pos in sorted({offset[:2] for offset in offsets}, key=lambda p: (-hops(p), p)):
            now = sorted((o for o in offsets if o[:2] == pos), key=hops, reverse=True)
            i, j, _ = at.moved(now[0], 1)
            compute(i * sizes[1] + j)
            for offset in now:
                start(sum_pair(held, routes, offset))
            if send:
                sum_send(held, routes, ready)
            ready = now
        if send:
            sum_send(held, routes, ready)

    def sum_finish(held, routes, stages=(1, 2, 3)):
        rest = [(route, offset) for route in routes for offset in offsets]
        rest = [r for r in rest if place_in(r[0][1], r[1], False) in stages]
        rest.sort(key=lambda r: (place_in(r[0][1], r[1], False), -hops(r[1])))
        for route, offset in rest:
            sum_block(held, route, offset)

    def by_owner(product):
        return product.astype(BF16).reshape(n_tp, tok_rows, product.shape[-1])

    def span_of(q):
        return pl.ds(pl.multiple_of(q * tile, tile), tile)

    def members_of(q):
        return pl.ds(q * n_tp, n_tp)

    def normalise(part, src):
        values = src[...].astype(F32)
        normed[part, at.me] = (values * inverse_rms(values) * pre_ref[...]).astype(BF16)

    def activations(part, q):
        tokens = normed[part, members_of(q)].reshape(tile, width)
        gate_tile = jnp.dot(tokens, all_rows(GATE), preferred_element_type=F32)
        up_tile = jnp.dot(tokens, all_rows(UP), preferred_element_type=F32)
        return gate_tile, up_tile, (gate_tile * jax.nn.sigmoid(gate_tile) * up_tile).astype(BF16)

    z, y, x = range(3)
    early_tokens, late_tokens = [(0, (z, y, x), 0, width)], [(1, (z, y, x), 0, width)]
    normed_sum, late_sum = [(2, (x, y, z), 0, width)], [(3, (x, y, z), 0, width)]

    def balanced(first, begin, size):
        routes, done = [], 0
        for i, order in enumerate(((x, y, z), (y, z, x), (z, x, y))):
            end = (i + 1) * (size // LANES) // 3 * LANES
            if end > done:
                col = begin + done
                col = col if isinstance(col, int) else pl.multiple_of(col, LANES)
                routes.append((first + i, order, col, end - done))
            done = end
        return routes

    cot_tokens = balanced(4, 0, width)

    def mixed_sum(dg):
        return balanced(7 + 3 * dg, at.at_g(dg) * chunk, chunk)

    with scope("enter"):
        at.enter()
    early_buf, late_buf = normed.at[EARLY], normed.at[LATE]
    with scope("issue"):
        for load in loads:
            load.wait()
        normalise(EARLY, early_ref)
        gather_start(early_buf, early_tokens)
        send_weights(GATE)
        normalise(LATE, late_ref)
        gather_start(late_buf, late_tokens)
        for w in range(3):
            own = pl.ds(pl.multiple_of(at.q * units, units), units)
            weights[w, at.fs] = w_refs[w][:, own]
    with scope("early_stage_0"):
        gather_pass_on(early_buf, early_tokens, [0])
        send_weights(UP)
    with scope("early_stage_1"):
        gather_pass_on(early_buf, early_tokens, [1])
    with scope("late_stage_0"):
        gather_pass_on(late_buf, late_tokens, [0])
        send_weights(DOWN)
    with scope("early_stage_2"):
        gather_pass_on(early_buf, early_tokens, [2])
    with scope("late_stage_1"):
        gather_pass_on(late_buf, late_tokens, [1])
    with scope("early_wait"):
        gather_wait(early_buf, early_tokens)
    with scope("gate_wait"):
        wait_weights(GATE, range(groups))
    with scope("up_wait"):
        wait_weights(UP, range(groups))

    with scope("early_forward"):

        @pl.loop(0, quad)
        def _(i):
            span = span_of(i)
            gate[span], up[span], hidden[span] = activations(EARLY, i)

    with scope("late_stage_2"):
        gather_pass_on(late_buf, late_tokens, [2])
        gather_wait(late_buf, late_tokens)
    with scope("late_hidden"):

        @pl.loop(0, quad)
        def _(i):
            hidden_late[span_of(i)] = activations(LATE, i)[2]

    def chunk_of(dg):
        return pl.ds(pl.multiple_of(at.at_g(dg) * chunk, chunk), chunk)

    first_mixed = len(pending)
    for dg in range(groups):
        with scope(f"down_wait_{dg}"):
            wait_weights(DOWN, [dg])

        def mixed_part(q, dg=dg):
            down = weights[DOWN, pl.ds(at.at_g(dg) * quad, quad)].reshape(chunk, units)
            parts[0, members_of(q), :, chunk_of(dg)] = by_owner(
                contract_last(hidden[span_of(q)], down)
            )

        with scope(f"mixed_{dg}"):
            sum_start(0, mixed_sum(dg), mixed_part)
    for stage in (1, 2, 3):
        with scope(f"mixed_finish_{stage}"):
            for dg in range(groups):
                sum_finish(0, mixed_sum(dg), [stage])
    mixed_sends = pending[first_mixed:]
    del pending[first_mixed:]
    with scope("mixed_cot"):
        mixed = total[...].astype(BF16).astype(F32)
        inverse = inverse_rms(mixed)
        weighted = 0.5 * grad_ref[...].astype(F32) * post_ref[...]
        cots[at.me] = (
            inverse * weighted
            - mixed * inverse**3 * jnp.mean(weighted * mixed, axis=-1, keepdims=True)
        ).astype(BF16)
        gather_start(cots, cot_tokens)

    def late_part(q):
        parts[1, members_of(q)] = by_owner(contract_last(hidden_late[span_of(q)], all_rows(DOWN)))

    with scope("late_sum"):
        sum_start(1, late_sum, late_part, send=False)
    with scope("cot_tokens"):
        gather_pass_on(cots, cot_tokens)
        gather_wait(cots, cot_tokens)

    def grad_copy(w, dg, dq):
        slot = at.slot(dg, dq)
        who = {"fs": slot, "tp": at.tp}
        return remote(
            grad_parts.at[w, slot],
            grad_in.at[w, dg, dq],
            g_send.at[w, dg, dq],
            g_recv.at[w, dg, dq],
            who,
        )

    def grad_part(w, left_ref, right_ref, dg):
        @pl.loop(0, quad)
        def _(dq):
            slot = at.slot(dg, dq)
            left = left_ref[:, :, pl.ds(pl.multiple_of(slot * rows, rows), rows)]
            left = left.reshape(quad * tile, rows)
            grad_parts[w, slot] = (grad_scale * contract_first(left, right_ref[...])).astype(BF16)

    far = range(1, groups)
    straight = [dq for dq in q_order if dq % sizes[1] == 0]
    crossing = [dq for dq in q_order if dq % sizes[1]]

    def send_grads(w, dgs, dqs):
        for dq in dqs:
            for dg in dgs:
                if dg or dq:
                    start(grad_copy(w, dg, dq))

    early_rows = normed.at[EARLY]
    def hidden_cots():
        @pl.loop(0, quad)
        def _(i):
            span = span_of(i)
            cot = cots[members_of(i)].reshape(tile, width)
            hidden_cot = jnp.dot(cot, all_rows(DOWN), preferred_element_type=F32)
            gate_tile, up_tile = gate[span], up[span]
            sigmoid = jax.nn.sigmoid(gate_tile)
            gate_cot[span] = (
                hidden_cot * up_tile * sigmoid * (1.0 + gate_tile * (1.0 - sigmoid))
            ).astype(BF16)
            up_cot[span] = (hidden_cot * gate_tile * sigmoid).astype(BF16)

    def normed_part(q):
        span = span_of(q)
        parts[0, members_of(q)] = by_owner(
            contract_last(gate_cot[span], all_rows(GATE))
            + contract_last(up_cot[span], all_rows(UP))
        )

    def normed_start():
        for copy in mixed_sends:
            copy.wait_send()
        sum_start(0, normed_sum, normed_part)

    def late_end():
        sum_finish(1, late_sum, [3])
        mixed = total[...].astype(BF16).astype(F32)
        late_out[...] = (
            late_ref[...].astype(F32) + 0.5 * mixed * inverse_rms(mixed) * post_ref[...]
        ).astype(BF16)

    def normed_end():
        sum_finish(0, normed_sum, [3])
        values = early_ref[...].astype(F32)
        inverse = inverse_rms(values)
        weighted = total[...].astype(BF16).astype(F32) * pre_ref[...]
        early_out[...] = (
            grad_ref[...].astype(F32)
            + inverse * weighted
            - values * inverse**3 * jnp.mean(weighted * values, axis=-1, keepdims=True)
        ).astype(BF16)

    operands_of = {DOWN: (cots, hidden), GATE: (early_rows, gate_cot), UP: (early_rows, up_cot)}

    def compute_grads(w, dgs):
        for dg in dgs:
            grad_part(w, *operands_of[w], dg)

    steps_by_name = {
        "late_send": lambda: sum_send(1, late_sum, offsets),
        "hidden_cots": hidden_cots,
        "normed_start": normed_start,
        "late_1": lambda: sum_finish(1, late_sum, [1]),
        "late_2": lambda: sum_finish(1, late_sum, [2]),
        "late_end": late_end,
        "normed_1": lambda: sum_finish(0, normed_sum, [1]),
        "normed_2": lambda: sum_finish(0, normed_sum, [2]),
        "normed_end": normed_end,
    }
    for name, w in (("down", DOWN), ("gate", GATE), ("up", UP)):
        for where, dgs in (("far", far), ("near", [0])):
            steps_by_name[f"{name}_{where}"] = functools.partial(compute_grads, w, dgs)
            for way, dqs in (("straight", straight), ("crossing", crossing)):
                steps_by_name[f"{name}_{where}_{way}"] = functools.partial(
                    send_grads, w, dgs, dqs
                )
    for name in LAST_PHASE:
        with scope(name):
            steps_by_name[name]()

    for w in (DOWN, GATE, UP):
        with scope(f"grad_out_{w}"):
            for dq in q_order:
                running = None
                for dg in range(groups):
                    if dg or dq:
                        grad_copy(w, dg, dq).wait_recv()
                        term = grad_in[w, dg, dq].astype(F32)
                    else:
                        term = grad_parts[w, at.fs].astype(F32)
                    running = term if running is None else running + term
                own = pl.ds(pl.multiple_of(at.at_q(-dq) * units, units), units)
                grad_outs[w][:, own] = running.astype(BF16)

    with scope("drain"):
        for copy in pending:
            copy.wait_send()


def per_device(
    n_fs,
    n_tp,
    late_input,
    early_input,
    early_grad,
    pre_gain,
    post_gain,
    gate_weight,
    up_weight,
    down_weight,
    gate_sum,
    up_sum,
    down_gradient_sum,
):
    tok_rows, width = late_input.shape
    rows, hidden_width = gate_weight.shape
    quad = quad_of(n_fs, n_tp)
    groups, members = n_fs // quad, quad * n_tp
    units = hidden_width // quad
    group_rows = members * tok_rows
    grad_scale = 1.0 / math.sqrt(tok_rows * n_tp * n_fs)
    dma = pltpu.SemaphoreType.DMA
    operands = (
        late_input,
        early_input,
        early_grad,
        pre_gain.reshape(1, width),
        post_gain.reshape(1, width),
        gate_weight,
        up_weight,
        down_weight,
    )
    outs = [jax.ShapeDtypeStruct((tok_rows, width), BF16)] * 2 + [
        jax.ShapeDtypeStruct((rows, hidden_width), BF16)
    ] * 3
    in_vmem = pl.BlockSpec(memory_space=pltpu.VMEM)
    late_output, early_input_grad, *grads = pl.pallas_call(
        functools.partial(layer_kernel, n_fs, n_tp, grad_scale),
        out_shape=outs,
        in_specs=[pl.BlockSpec(memory_space=pltpu.HBM)] * len(operands),
        out_specs=[in_vmem] * len(outs),
        scratch_shapes=[
            pltpu.VMEM((2, members, tok_rows, width), BF16),
            pltpu.VMEM((3, n_fs, rows, units), BF16),
            pltpu.VMEM((group_rows, units), F32),
            pltpu.VMEM((group_rows, units), F32),
            pltpu.VMEM((group_rows, units), BF16),
            pltpu.VMEM((members, tok_rows, width), BF16),
            pltpu.VMEM((2, members, tok_rows, width), BF16),
            pltpu.VMEM((2, members // PAIR, tok_rows, width), BF16),
            pltpu.VMEM((2, members // PAIR, tok_rows, width), BF16),
            pltpu.VMEM((tok_rows, width), F32),
            pltpu.VMEM((group_rows, units), BF16),
            pltpu.VMEM((group_rows, units), BF16),
            pltpu.VMEM((3, n_fs, rows, units), BF16),
            pltpu.VMEM((3, groups, quad, rows, units), BF16),
            pltpu.VMEM((group_rows, units), BF16),
        ]
        + [pltpu.VMEM(array.shape, array.dtype) for array in operands]
        + [dma((3, groups, quad))] * 4
        + [dma((7 + 3 * groups, 4, members // PAIR)), dma((len(operands),))],
        cost_estimate=pl.CostEstimate(flops=10**9, bytes_accessed=0, transcendentals=0),
        compiler_params=pltpu.CompilerParams(
            collective_id=0, has_side_effects=True, vmem_limit_bytes=VMEM_LIMIT
        ),
    )(*[pltpu.with_memory_space_constraint(array, pltpu.HBM) for array in operands])
    totals = [
        running + grad.astype(F32)
        for running, grad in zip((gate_sum, up_sum, down_gradient_sum), grads)
    ]
    return (late_output, early_input_grad, *totals)


def solution(mesh):
    in_specs = (
        P(("fs", "tp"), None),
        P(("fs", "tp"), None),
        P(("fs", "tp"), None),
        P(),
        P(),
        P("fs", "tp"),
        P("fs", "tp"),
        P("fs", "tp"),
        P("fs", "tp"),
        P("fs", "tp"),
        P("fs", "tp"),
    )
    out_specs = (
        P(("fs", "tp"), None),
        P(("fs", "tp"), None),
        P("fs", "tp"),
        P("fs", "tp"),
        P("fs", "tp"),
    )
    return jax.shard_map(
        functools.partial(per_device, mesh.shape["fs"], mesh.shape["tp"]),
        mesh=mesh, in_specs=in_specs, out_specs=out_specs, check_vma=False
    )
```

```python
import functools
import math

import jax
import jax.numpy as jnp
from jax import lax
from jax.experimental import pallas as pl
from jax.experimental.pallas import tpu as pltpu
from jax.sharding import PartitionSpec as P

NORM_EPS = 1e-06
PAIR = 2
GROUP = 16
LATE, EARLY = 0, 1
GATE, UP, DOWN = 0, 1, 2
MESH = pl.DeviceIdType.MESH
VMEM_LIMIT = 46 * 1024 * 1024
LANES = 128
BF16, F32 = jnp.bfloat16, jnp.float32
scope = jax.named_scope
LAST_PHASE = (
    "down_far", "down_far_crossing", "late_send", "down_near", "down_near_crossing",
    "down_far_straight", "hidden_cots", "gate_far", "gate_far_crossing", "gate_near",
    "gate_near_crossing", "up_far", "gate_far_straight", "normed_start", "up_near", "late_1",
    "up_far_straight", "down_near_straight", "up_near_crossing", "late_2",
    "gate_near_straight", "normed_1", "up_far_crossing", "up_near_straight", "normed_2",
    "late_end", "normed_end",
)


def contract_last(first_op, second_op):
    return lax.dot_general(
        first_op, second_op, (((1,), (1,)), ((), ())), preferred_element_type=F32
    )


def contract_first(first_op, second_op):
    return lax.dot_general(
        first_op, second_op, (((0,), (0,)), ((), ())), preferred_element_type=F32
    )


def inverse_rms(values):
    return lax.rsqrt(jnp.mean(values * values, axis=-1, keepdims=True) + NORM_EPS)


def quad_of(n_fs, n_tp):
    return min(n_fs, max(1, GROUP // n_tp))


def shape_of(n_fs, n_tp):
    quad = quad_of(n_fs, n_tp)
    deep = PAIR if quad % PAIR == 0 else 1
    return quad // deep, deep, n_tp // PAIR


class Place:
    def __init__(self, n_fs, n_tp):
        self.n_fs, self.n_tp = n_fs, n_tp
        self.quad = quad_of(n_fs, n_tp)
        self.groups = n_fs // self.quad
        self.sizes = shape_of(n_fs, n_tp)
        self.fs, self.tp = lax.axis_index("fs"), lax.axis_index("tp")
        self.g, self.q = self.fs // self.quad, self.fs % self.quad
        self.core = self.tp % PAIR
        self.coords = (self.q // self.sizes[1], self.q % self.sizes[1], self.tp // PAIR)
        self.offsets = [
            (i, j, k)
            for i in range(self.sizes[0])
            for j in range(self.sizes[1])
            for k in range(self.sizes[2])
        ]
        self.me = self.member((0, 0, 0), 1, self.core)
        self.partner = self.device((0, 0, 0), 1 - self.core)

    def moved(self, offset, sign):
        return [
            (c + size + sign * o) % size
            for c, size, o in zip(self.coords, self.sizes, offset)
        ]

    def member(self, offset, sign, core):
        i, j, k = self.moved(offset, sign)
        return (i * self.sizes[1] + j) * self.n_tp + k * PAIR + core

    def device(self, offset, core):
        i, j, k = self.moved(offset, 1)
        return {"fs": self.g * self.quad + i * self.sizes[1] + j, "tp": k * PAIR + core}

    def flat(self, offset):
        return (offset[0] * self.sizes[1] + offset[1]) * self.sizes[2] + offset[2]

    def at_q(self, dq):
        return (self.q + self.quad + dq) % self.quad

    def at_g(self, dg):
        return (self.g + dg) % self.groups

    def slot(self, dg, dq):
        return self.at_g(dg) * self.quad + self.at_q(dq)

    def enter(self):
        barrier = pltpu.get_barrier_semaphore()

        def greet(fs, tp):
            pl.semaphore_signal(
                barrier, inc=1, device_id={"fs": fs, "tp": tp}, device_id_type=MESH
            )

        peers = 0
        for offset in range(1, self.n_fs):
            greet((self.fs + offset) % self.n_fs, self.tp)
            peers += 1
        for dq in range(self.quad):
            for offset in range(1, self.n_tp):
                greet(self.g * self.quad + self.at_q(dq), (self.tp + offset) % self.n_tp)
                peers += 1
        pl.semaphore_wait(barrier, peers)


def remote(src, dst, send_sem, recv_sem, who):
    return pltpu.make_async_remote_copy(
        src_ref=src,
        dst_ref=dst,
        send_sem=send_sem,
        recv_sem=recv_sem,
        device_id=who,
        device_id_type=MESH,
    )


def layer_kernel(n_fs, n_tp, grad_scale, *refs):
    sources = refs[:8]
    late_out, early_out = refs[8:10]
    grad_outs = refs[10:13]
    normed, weights, gate, up, hidden, cots, parts, pair_in, sums_in, total = refs[13:23]
    gate_cot, up_cot, grad_parts, grad_in, hidden_late = refs[23:28]
    late_ref, early_ref, grad_ref, pre_ref, post_ref = refs[28:33]
    w_refs = refs[33:36]
    w_send, w_recv, g_send, g_recv, sems, load_sem = refs[36:]
    loads = [
        pltpu.make_async_copy(src, dst, load_sem.at[i])
        for i, (src, dst) in enumerate(zip(sources, refs[28:36]))
    ]
    for i in (1, 3, 5, 0, 6, 7, 2, 4):
        loads[i].start()

    at = Place(n_fs, n_tp)
    quad, groups, sizes, offsets = at.quad, at.groups, at.sizes, at.offsets
    home, others = offsets[0], offsets[1:]
    tok_rows, width = early_ref.shape
    rows, units = weights.shape[2:]
    tile = n_tp * tok_rows
    chunk = quad * rows
    pending = []

    def start(copy):
        copy.start()
        pending.append(copy)

    def w_copy(w, dg, dq):
        source = w_refs[w].at[:, pl.ds(pl.multiple_of(at.at_q(dq) * units, units), units)]
        who = {"fs": at.slot(dg, dq), "tp": at.tp}
        return remote(
            source, weights.at[w, at.fs], w_send.at[w, dg, dq], w_recv.at[w, dg, dq], who
        )

    q_order = [1, 3, 2, 0] if quad == 4 else list(range(quad - 1, -1, -1))

    def send_weights(w):
        for dq in q_order:
            for dg in range(groups - 1, -1, -1):
                if dg or dq:
                    start(w_copy(w, dg, dq))

    def wait_weights(w, dgs):
        for dg in dgs:
            for dq in q_order:
                if dg or dq:
                    w_copy(w, dg, dq).wait_recv()

    def all_rows(w):
        return weights[w].reshape(n_fs * rows, units)

    def place_in(order, offset, last):
        found = [p for p, axis in enumerate(order) if offset[axis]]
        if not found:
            return -1 if last else len(order)
        return found[-1] if last else found[0]

    def put(offset, axis, value):
        return tuple(value if i == axis else o for i, o in enumerate(offset))

    def along(offset, axis):
        return tuple(o if i == axis else 0 for i, o in enumerate(offset))

    def steps(axis):
        return range(1, sizes[axis])

    def hops(offset):
        return sum(1 for o in offset if o)

    def cols_of(route):
        return pl.ds(route[2], route[3])

    def ici(inst, offset, src, dst, who):
        i = at.flat(offset)
        return remote(src, dst, sems.at[inst, 0, i], sems.at[inst, 1, i], who)

    def pair(inst, offset, src, dst):
        i = at.flat(offset)
        return remote(src, dst, sems.at[inst, 2, i], sems.at[inst, 3, i], at.partner)

    def gather_copy(buf, route, offset):
        axis = route[1][place_in(route[1], offset, True)]
        block = buf.at[at.member(put(offset, axis, 0), -1, at.core), :, cols_of(route)]
        return ici(route[0], offset, block, block, at.device(along(offset, axis), at.core))

    def gather_pair(buf, route, offset):
        block = buf.at[at.member(offset, -1, at.core), :, cols_of(route)]
        return pair(route[0], offset, block, block)

    def onward(route, offset):
        order = route[1]
        later = order[place_in(order, offset, True) + 1 :]
        return [put(offset, axis, e) for axis in later for e in steps(axis)]

    def gather_start(buf, routes):
        sends = [(route, offset) for route in routes for offset in onward(route, home)]
        sends.sort(key=lambda send: place_in(send[0][1], send[1], True))
        for route, offset in sends:
            start(gather_copy(buf, route, offset))
        for route in routes:
            start(gather_pair(buf, route, home))

    def gather_pass_on(buf, routes, stages=range(3)):
        arrivals = [(route, offset) for route in routes for offset in others]
        arrivals = [a for a in arrivals if place_in(a[0][1], a[1], True) in stages]
        arrivals.sort(key=lambda a: (hops(a[1]), place_in(a[0][1], a[1], True)))
        for route, offset in arrivals:
            gather_copy(buf, route, offset).wait_recv()
            for further in onward(route, offset):
                start(gather_copy(buf, route, further))
            start(gather_pair(buf, route, offset))

    def gather_wait(buf, routes):
        for route in routes:
            for offset in offsets:
                gather_pair(buf, route, offset).wait_recv()

    def sum_pair(held, routes, offset):
        cols = pl.ds(routes[0][2], sum(route[3] for route in routes))
        return pair(
            routes[0][0],
            offset,
            parts.at[held, at.member(offset, 1, 1 - at.core), :, cols],
            pair_in.at[held, at.flat(offset), :, cols],
        )

    def sum_copy(held, route, offset):
        axis = route[1][place_in(route[1], offset, False)]
        return ici(
            route[0],
            offset,
            parts.at[held, at.member(offset, 1, at.core), :, cols_of(route)],
            sums_in.at[held, at.flat(offset), :, cols_of(route)],
            at.device(along(offset, axis), at.core),
        )

    def sum_block(held, route, offset):
        cols, mine = cols_of(route), at.member(offset, 1, at.core)
        running = parts[held, mine, :, cols].astype(F32)
        running = running + pair_in[held, at.flat(offset), :, cols].astype(F32)
        for axis in route[1][: place_in(route[1], offset, False)]:
            for e in steps(axis):
                came = put(offset, axis, e)
                sum_copy(held, route, came).wait_recv()
                running = running + sums_in[held, at.flat(came), :, cols].astype(F32)
        if offset == home:
            total[:, cols] = running
        else:
            parts[held, mine, :, cols] = running.astype(BF16)
            start(sum_copy(held, route, offset))

    def sum_send(held, routes, ready):
        for offset in ready:
            sum_pair(held, routes, offset).wait_recv()
        for route in routes:
            for offset in ready:
                if place_in(route[1], offset, False) == 0:
                    sum_block(held, route, offset)

    def sum_start(held, routes, compute, send=True):
        ready = []
        for pos in sorted({offset[:2] for offset in offsets}, key=lambda p: (-hops(p), p)):
            now = sorted((o for o in offsets if o[:2] == pos), key=hops, reverse=True)
            i, j, _ = at.moved(now[0], 1)
            compute(i * sizes[1] + j)
            for offset in now:
                start(sum_pair(held, routes, offset))
            if send:
                sum_send(held, routes, ready)
            ready = now
        if send:
            sum_send(held, routes, ready)

    def sum_finish(held, routes, stages=(1, 2, 3)):
        rest = [(route, offset) for route in routes for offset in offsets]
        rest = [r for r in rest if place_in(r[0][1], r[1], False) in stages]
        rest.sort(key=lambda r: (place_in(r[0][1], r[1], False), -hops(r[1])))
        for route, offset in rest:
            sum_block(held, route, offset)

    def by_owner(product):
        return product.astype(BF16).reshape(n_tp, tok_rows, product.shape[-1])

    def span_of(q):
        return pl.ds(pl.multiple_of(q * tile, tile), tile)

    def members_of(q):
        return pl.ds(q * n_tp, n_tp)

    def normalise(part, src):
        values = src[...].astype(F32)
        normed[part, at.me] = (values * inverse_rms(values) * pre_ref[...]).astype(BF16)

    def activations(part, q):
        tokens = normed[part, members_of(q)].reshape(tile, width)
        gate_tile = jnp.dot(tokens, all_rows(GATE), preferred_element_type=F32)
        up_tile = jnp.dot(tokens, all_rows(UP), preferred_element_type=F32)
        return gate_tile, up_tile, (gate_tile * jax.nn.sigmoid(gate_tile) * up_tile).astype(BF16)

    z, y, x = range(3)
    early_tokens, late_tokens = [(0, (z, y, x), 0, width)], [(1, (z, y, x), 0, width)]
    normed_sum, late_sum = [(2, (x, y, z), 0, width)], [(3, (x, y, z), 0, width)]

    def balanced(first, begin, size):
        routes, done = [], 0
        for i, order in enumerate(((x, y, z), (y, z, x), (z, x, y))):
            end = (i + 1) * (size // LANES) // 3 * LANES
            if end > done:
                col = begin + done
                col = col if isinstance(col, int) else pl.multiple_of(col, LANES)
                routes.append((first + i, order, col, end - done))
            done = end
        return routes

    cot_tokens = balanced(4, 0, width)

    def mixed_sum(dg):
        return balanced(7 + 3 * dg, at.at_g(dg) * chunk, chunk)

    with scope("enter"):
        at.enter()
    early_buf, late_buf = normed.at[EARLY], normed.at[LATE]
    with scope("issue"):
        for load in loads:
            load.wait()
        normalise(EARLY, early_ref)
        gather_start(early_buf, early_tokens)
        send_weights(GATE)
        normalise(LATE, late_ref)
        gather_start(late_buf, late_tokens)
        for w in range(3):
            own = pl.ds(pl.multiple_of(at.q * units, units), units)
            weights[w, at.fs] = w_refs[w][:, own]
    with scope("early_stage_0"):
        gather_pass_on(early_buf, early_tokens, [0])
        send_weights(UP)
    with scope("early_stage_1"):
        gather_pass_on(early_buf, early_tokens, [1])
    with scope("late_stage_0"):
        gather_pass_on(late_buf, late_tokens, [0])
        send_weights(DOWN)
    with scope("early_stage_2"):
        gather_pass_on(early_buf, early_tokens, [2])
    with scope("late_stage_1"):
        gather_pass_on(late_buf, late_tokens, [1])
    with scope("early_wait"):
        gather_wait(early_buf, early_tokens)
    with scope("gate_wait"):
        wait_weights(GATE, range(groups))
    with scope("up_wait"):
        wait_weights(UP, range(groups))

    with scope("early_forward"):

        @pl.loop(0, quad)
        def _(i):
            span = span_of(i)
            gate[span], up[span], hidden[span] = activations(EARLY, i)

    with scope("late_stage_2"):
        gather_pass_on(late_buf, late_tokens, [2])
        gather_wait(late_buf, late_tokens)
    with scope("late_hidden"):

        @pl.loop(0, quad)
        def _(i):
            hidden_late[span_of(i)] = activations(LATE, i)[2]

    def chunk_of(dg):
        return pl.ds(pl.multiple_of(at.at_g(dg) * chunk, chunk), chunk)

    first_mixed = len(pending)
    for dg in range(groups):
        with scope(f"down_wait_{dg}"):
            wait_weights(DOWN, [dg])

        def mixed_part(q, dg=dg):
            down = weights[DOWN, pl.ds(at.at_g(dg) * quad, quad)].reshape(chunk, units)
            parts[0, members_of(q), :, chunk_of(dg)] = by_owner(
                contract_last(hidden[span_of(q)], down)
            )

        with scope(f"mixed_{dg}"):
            sum_start(0, mixed_sum(dg), mixed_part)
    for stage in (1, 2, 3):
        with scope(f"mixed_finish_{stage}"):
            for dg in range(groups):
                sum_finish(0, mixed_sum(dg), [stage])
    mixed_sends = pending[first_mixed:]
    del pending[first_mixed:]
    with scope("mixed_cot"):
        mixed = total[...].astype(BF16).astype(F32)
        inverse = inverse_rms(mixed)
        weighted = 0.5 * grad_ref[...].astype(F32) * post_ref[...]
        cots[at.me] = (
            inverse * weighted
            - mixed * inverse**3 * jnp.mean(weighted * mixed, axis=-1, keepdims=True)
        ).astype(BF16)
        gather_start(cots, cot_tokens)

    def late_part(q):
        parts[1, members_of(q)] = by_owner(contract_last(hidden_late[span_of(q)], all_rows(DOWN)))

    with scope("late_sum"):
        sum_start(1, late_sum, late_part, send=False)
    with scope("cot_tokens"):
        gather_pass_on(cots, cot_tokens)
        gather_wait(cots, cot_tokens)

    def grad_copy(w, dg, dq):
        slot = at.slot(dg, dq)
        who = {"fs": slot, "tp": at.tp}
        return remote(
            grad_parts.at[w, slot],
            grad_in.at[w, dg, dq],
            g_send.at[w, dg, dq],
            g_recv.at[w, dg, dq],
            who,
        )

    def grad_part(w, left_ref, right_ref, dg):
        @pl.loop(0, quad)
        def _(dq):
            slot = at.slot(dg, dq)
            left = left_ref[:, :, pl.ds(pl.multiple_of(slot * rows, rows), rows)]
            left = left.reshape(quad * tile, rows)
            grad_parts[w, slot] = (grad_scale * contract_first(left, right_ref[...])).astype(BF16)

    far = range(1, groups)
    straight = [dq for dq in q_order if dq % sizes[1] == 0]
    crossing = [dq for dq in q_order if dq % sizes[1]]

    def send_grads(w, dgs, dqs):
        for dq in dqs:
            for dg in dgs:
                if dg or dq:
                    start(grad_copy(w, dg, dq))

    early_rows = normed.at[EARLY]
    def hidden_cots():
        @pl.loop(0, quad)
        def _(i):
            span = span_of(i)
            cot = cots[members_of(i)].reshape(tile, width)
            hidden_cot = jnp.dot(cot, all_rows(DOWN), preferred_element_type=F32)
            gate_tile, up_tile = gate[span], up[span]
            sigmoid = jax.nn.sigmoid(gate_tile)
            gate_cot[span] = (
                hidden_cot * up_tile * sigmoid * (1.0 + gate_tile * (1.0 - sigmoid))
            ).astype(BF16)
            up_cot[span] = (hidden_cot * gate_tile * sigmoid).astype(BF16)

    def normed_part(q):
        span = span_of(q)
        parts[0, members_of(q)] = by_owner(
            contract_last(gate_cot[span], all_rows(GATE))
            + contract_last(up_cot[span], all_rows(UP))
        )

    def normed_start():
        for copy in mixed_sends:
            copy.wait_send()
        sum_start(0, normed_sum, normed_part)

    def late_end():
        sum_finish(1, late_sum, [3])
        mixed = total[...].astype(BF16).astype(F32)
        late_out[...] = (
            late_ref[...].astype(F32) + 0.5 * mixed * inverse_rms(mixed) * post_ref[...]
        ).astype(BF16)

    def normed_end():
        sum_finish(0, normed_sum, [3])
        values = early_ref[...].astype(F32)
        inverse = inverse_rms(values)
        weighted = total[...].astype(BF16).astype(F32) * pre_ref[...]
        early_out[...] = (
            grad_ref[...].astype(F32)
            + inverse * weighted
            - values * inverse**3 * jnp.mean(weighted * values, axis=-1, keepdims=True)
        ).astype(BF16)

    operands_of = {DOWN: (cots, hidden), GATE: (early_rows, gate_cot), UP: (early_rows, up_cot)}

    def compute_grads(w, dgs):
        for dg in dgs:
            grad_part(w, *operands_of[w], dg)

    steps_by_name = {
        "late_send": lambda: sum_send(1, late_sum, offsets),
        "hidden_cots": hidden_cots,
        "normed_start": normed_start,
        "late_1": lambda: sum_finish(1, late_sum, [1]),
        "late_2": lambda: sum_finish(1, late_sum, [2]),
        "late_end": late_end,
        "normed_1": lambda: sum_finish(0, normed_sum, [1]),
        "normed_2": lambda: sum_finish(0, normed_sum, [2]),
        "normed_end": normed_end,
    }
    for name, w in (("down", DOWN), ("gate", GATE), ("up", UP)):
        for where, dgs in (("far", far), ("near", [0])):
            steps_by_name[f"{name}_{where}"] = functools.partial(compute_grads, w, dgs)
            for way, dqs in (("straight", straight), ("crossing", crossing)):
                steps_by_name[f"{name}_{where}_{way}"] = functools.partial(
                    send_grads, w, dgs, dqs
                )
    for name in LAST_PHASE:
        with scope(name):
            steps_by_name[name]()

    for w in (DOWN, GATE, UP):
        with scope(f"grad_out_{w}"):
            for dq in q_order:
                running = None
                for dg in range(groups):
                    if dg or dq:
                        grad_copy(w, dg, dq).wait_recv()
                        term = grad_in[w, dg, dq].astype(F32)
                    else:
                        term = grad_parts[w, at.fs].astype(F32)
                    running = term if running is None else running + term
                own = pl.ds(pl.multiple_of(at.at_q(-dq) * units, units), units)
                grad_outs[w][:, own] = running.astype(BF16)

    with scope("drain"):
        for copy in pending:
            copy.wait_send()


def per_device(
    n_fs,
    n_tp,
    late_input,
    early_input,
    early_grad,
    pre_gain,
    post_gain,
    gate_weight,
    up_weight,
    down_weight,
    gate_sum,
    up_sum,
    down_gradient_sum,
):
    tok_rows, width = late_input.shape
    rows, hidden_width = gate_weight.shape
    quad = quad_of(n_fs, n_tp)
    groups, members = n_fs // quad, quad * n_tp
    units = hidden_width // quad
    group_rows = members * tok_rows
    grad_scale = 1.0 / math.sqrt(tok_rows * n_tp * n_fs)
    dma = pltpu.SemaphoreType.DMA
    operands = (
        late_input,
        early_input,
        early_grad,
        pre_gain.reshape(1, width),
        post_gain.reshape(1, width),
        gate_weight,
        up_weight,
        down_weight,
    )
    outs = [jax.ShapeDtypeStruct((tok_rows, width), BF16)] * 2 + [
        jax.ShapeDtypeStruct((rows, hidden_width), BF16)
    ] * 3
    in_vmem = pl.BlockSpec(memory_space=pltpu.VMEM)
    late_output, early_input_grad, *grads = pl.pallas_call(
        functools.partial(layer_kernel, n_fs, n_tp, grad_scale),
        out_shape=outs,
        in_specs=[pl.BlockSpec(memory_space=pltpu.HBM)] * len(operands),
        out_specs=[in_vmem] * len(outs),
        scratch_shapes=[
            pltpu.VMEM((2, members, tok_rows, width), BF16),
            pltpu.VMEM((3, n_fs, rows, units), BF16),
            pltpu.VMEM((group_rows, units), F32),
            pltpu.VMEM((group_rows, units), F32),
            pltpu.VMEM((group_rows, units), BF16),
            pltpu.VMEM((members, tok_rows, width), BF16),
            pltpu.VMEM((2, members, tok_rows, width), BF16),
            pltpu.VMEM((2, members // PAIR, tok_rows, width), BF16),
            pltpu.VMEM((2, members // PAIR, tok_rows, width), BF16),
            pltpu.VMEM((tok_rows, width), F32),
            pltpu.VMEM((group_rows, units), BF16),
            pltpu.VMEM((group_rows, units), BF16),
            pltpu.VMEM((3, n_fs, rows, units), BF16),
            pltpu.VMEM((3, groups, quad, rows, units), BF16),
            pltpu.VMEM((group_rows, units), BF16),
        ]
        + [pltpu.VMEM(array.shape, array.dtype) for array in operands]
        + [dma((3, groups, quad))] * 4
        + [dma((7 + 3 * groups, 4, members // PAIR)), dma((len(operands),))],
        cost_estimate=pl.CostEstimate(flops=10**9, bytes_accessed=0, transcendentals=0),
        compiler_params=pltpu.CompilerParams(
            collective_id=0, has_side_effects=True, vmem_limit_bytes=VMEM_LIMIT
        ),
    )(*[pltpu.with_memory_space_constraint(array, pltpu.HBM) for array in operands])
    totals = [
        running + grad.astype(F32)
        for running, grad in zip((gate_sum, up_sum, down_gradient_sum), grads)
    ]
    return (late_output, early_input_grad, *totals)


def solution(mesh):
    in_specs = (
        P(("fs", "tp"), None),
        P(("fs", "tp"), None),
        P(("fs", "tp"), None),
        P(),
        P(),
        P("fs", "tp"),
        P("fs", "tp"),
        P("fs", "tp"),
        P("fs", "tp"),
        P("fs", "tp"),
        P("fs", "tp"),
    )
    out_specs = (
        P(("fs", "tp"), None),
        P(("fs", "tp"), None),
        P("fs", "tp"),
        P("fs", "tp"),
        P("fs", "tp"),
    )
    return jax.shard_map(
        functools.partial(per_device, mesh.shape["fs"], mesh.shape["tp"]),
        mesh=mesh, in_specs=in_specs, out_specs=out_specs, check_vma=False
    )
```
